128 devices in a mesh: sp: 64 (over z, y, x), tp: 2 (over core).
Axes of the slice: x: 4, y: 4, z: 4, core: 2. Of those that a mesh axis runs over, the one named last changes fastest.
Arguments:
- residual: bfloat16 [16384, 2048], P(('sp', 'tp')), may hold values from -6 to 6
- query_nope: bfloat16 [16384, 1024], P('sp', 'tp'), may hold values from -24 to 24
- query_rope: bfloat16 [16384, 512], P('sp', 'tp'), may hold values from -400 to 400
- latent: bfloat16 [16384, 256], P(('sp', 'tp')), may hold values from -6 to 6
- key_rope: bfloat16 [16384, 64], P(('sp', 'tp')), may hold values from -6 to 6
- key_up: bfloat16 [256, 1024], P(None, 'tp'), may hold values from -0.375 to 0.375
- value_up: bfloat16 [256, 1024], P(None, 'tp'), may hold values from -0.375 to 0.375
- out_proj: bfloat16 [1024, 2048], replicated, may hold values from -0.375 to 0.375
- norm_gain: float32 [2048], replicated, may hold values from 0.1 to 1.9
- routes: int32 [16384, 2], P(('sp', 'tp')), may hold values from 0 to 63, all different within a row; in each aligned block of 128 rows (0 to 127, 128 to 255, ...) at most 8 rows name the same one
- route_weight: float32 [16384, 2], P(('sp', 'tp')), may hold values from 0.3 to 2.5
- w_gate: bfloat16 [64, 2048, 512], P('sp', None, 'tp'), may hold values from -0.125 to 0.125
- w_up: bfloat16 [64, 2048, 512], P('sp', None, 'tp'), may hold values from -0.125 to 0.125
- w_down: bfloat16 [64, 512, 2048], P('sp', 'tp'), may hold values from -0.25 to 0.25
Outputs:
- mixed: bfloat16 [16384, 2048], P(('sp', 'tp'))
The draws below stay inside these ranges and needn't reach their ends.
Inputs may be any that keep to these rules, and one draw needn't show every extreme that they name: `routes`: each row names 2 different experts. Among the rows of one device no expert is named more than 8 times, a bound that some block reaches by the rows of some device.
All inputs are finite; a program needn't handle non-finite values.
Results may differ from the reference program's by a relative error of at most 0.015.
Values may be sent and summed in bfloat16 or wider, within the bound.
A program may use at most 128 MiB of HBM per device.

```python
import math
import jax
import jax.numpy as jnp
import numpy as np
from jax import lax

D = 2048
HEADS = 8
QK_NOPE = 128
QK_ROPE = 64
V_DIM = 128
LATENT = 256
FF = 512
TOP = 2
SEGMENT = 64
TOK_DEV = 256
TOKENS = 16384
EXPERTS = 64
CAP = 8
N_SP = 64
N_TP = 2


def draw_key_rope(key, part):
    noise = jax.random.truncated_normal(jax.random.fold_in(key, 31), -6.0, 6.0, (TOKENS, QK_ROPE), jnp.float32)
    return noise.astype(jnp.bfloat16)


def draw_query_rope(key, part):
    noise = jax.random.truncated_normal(jax.random.fold_in(key, 32), -6.0, 6.0, (TOKENS, HEADS * QK_ROPE), jnp.float32)
    return noise.astype(jnp.bfloat16)


def steps_of(rng, dims, shards, low, largest):
    loudness, own = 1.0, jax.random.fold_in(rng, 6)
    for dim, blocks in shards:
        heights = jnp.exp(jax.random.uniform(jax.random.fold_in(own, dim), (blocks,), jnp.float32, low / len(shards), largest / len(shards)))
        loudness = loudness * jnp.repeat(heights, dims[dim] // blocks).reshape([-1 if axis == dim else 1 for axis in range(len(dims))])
    return loudness


def routed_block(key, own, number, rows, number_of, top, reach, skew):
    order = jax.random.permutation(key, number_of)
    crowded, usual = load_shares(number_of, rows * top, reach, skew, True), load_shares(number_of, rows * top, reach, skew, False)
    places = jnp.arange(number_of)

    def named(sizes, turn):
        used = int((sizes > 0).sum())
        fixed = max(1, used // 4)
        moved = fixed + (places - fixed + turn * (used - fixed)) % max(1, number_of - fixed)
        return jnp.zeros((number_of,), jnp.int32).at[order[jnp.where(places < fixed, places, moved)]].set(jnp.asarray(sizes, jnp.int32))

    sizes = jnp.where(number % 4 == 0, named(crowded, number // 4), named(usual, number - number // 4 - 1))
    mixed = jax.random.permutation(jax.random.fold_in(own, 3), number_of)
    donor, taker = mixed[0:number_of // 2 * 2:2], mixed[1:number_of // 2 * 2:2]
    slack = jnp.minimum(sizes[donor] - 1, reach - sizes[taker]) // 2
    slack = jnp.where((donor == order[0]) | (taker == order[0]) | (sizes[taker] == 0), 0, jnp.maximum(slack, 0))
    moved = jax.random.randint(jax.random.fold_in(own, 4), (number_of // 2,), 0, 1 << 20) % (slack + 1)
    sizes = sizes.at[donor].add(-moved).at[taker].add(moved)
    items = jnp.searchsorted(jnp.cumsum(sizes), jnp.arange(rows * top), side="right").astype(jnp.int32)
    grid = items.reshape(top, rows).T
    grid = grid[jax.random.permutation(jax.random.fold_in(own, 1), rows)]
    turn = jax.random.randint(jax.random.fold_in(own, 2), (rows, 1), 0, top)
    return jnp.take_along_axis(grid, (jnp.arange(top)[None, :] + turn) % top, axis=1)


def load_shares(count, total, most, slope, full):
    weights = [(1 << 20) // math.isqrt(standing ** slope) + 1 for standing in range(1, count + 1)]
    largest = most if full else min(most, max(-(-total // count), total * weights[0] // sum(weights)))
    least = 1 if total - largest >= count - 1 else 0
    holding, surplus = [largest] + [least] * (count - 1), total - largest - least * (count - 1)
    while surplus > 0:
        movable = [i for i in range(1, count) if holding[i] < largest] or [i for i in range(1, count) if holding[i] < most]
        whole, budget = sum([weights[i] for i in movable]), surplus
        for i in movable:
            addition = min(most - holding[i], max(1, budget * weights[i] // whole), surplus)
            holding[i] = holding[i] + addition
            surplus = surplus - addition
    return np.array(holding)


def normal_values(own_key, shape, width, most, split=(), held_as=jnp.bfloat16):
    values = jax.random.normal(own_key, shape, jnp.float32) * width
    if len(split) > 0:
        values = steps_of(own_key, shape, split, -0.22, 0.18) * values
    return jnp.clip(values, min=-most, max=most).astype(held_as)


def setup_inputs(seed: int = 0) -> dict:
    keys = jax.random.split(jax.random.key(seed), 15)
    residual = normal_values(keys[0], (TOKENS, D), 1.0, 6.0, ((0, 128),))
    query_nope = normal_values(keys[1], (TOKENS, HEADS * QK_NOPE), 4.0, 24.0, ((0, 64), (1, 2)))
    query_rope = draw_query_rope(jax.random.fold_in(keys[14], 71), 0)
    latent = normal_values(keys[3], (TOKENS, LATENT), 1.0, 6.0, ((0, 128),))
    key_rope = draw_key_rope(jax.random.fold_in(keys[14], 71), 0)
    key_up = normal_values(keys[5], (LATENT, HEADS * QK_NOPE), LATENT ** -0.5, 0.375, ((1, 2),))
    value_up = normal_values(keys[6], (LATENT, HEADS * V_DIM), LATENT ** -0.5, 0.375, ((1, 2),))
    out_proj = normal_values(keys[7], (HEADS * V_DIM, D), (HEADS * V_DIM // 4) ** -0.5, 0.375)
    norm_gain = jnp.clip(1.0 + 0.18 * jax.random.normal(keys[8], (D,), jnp.float32), 0.1, 1.9)
    routes_keys = jax.random.split(jax.random.fold_in(keys[9], 1), TOKENS // (TOK_DEV // N_TP))
    routes_turns = jax.random.permutation(jax.random.fold_in(keys[9], 3), TOKENS // (TOK_DEV // N_TP))
    routes = jax.vmap(lambda own, number: routed_block(jax.random.fold_in(keys[9], 2), own, number, TOK_DEV // N_TP, EXPERTS, TOP, CAP, 2))(routes_keys, routes_turns).reshape((TOKENS, TOP))
    route_weight = jnp.clip(jnp.exp(math.log(2.5) - 2.1202635 * jax.random.uniform(keys[10], (TOKENS, TOP), jnp.float32) ** steps_of(keys[10], (TOKENS, TOP), ((0, 128),), -0.2, 0.2)), 0.3, 2.5)
    w_gate = normal_values(keys[11], (EXPERTS, D, FF), D ** -0.5, 0.125, ((0, 64), (2, 2)))
    w_up = normal_values(keys[12], (EXPERTS, D, FF), D ** -0.5, 0.125, ((0, 64), (2, 2)))
    w_down = normal_values(keys[13], (EXPERTS, FF, D), FF ** -0.5, 0.25, ((0, 64), (1, 2)))
    return dict(residual=residual, query_nope=query_nope, query_rope=query_rope, latent=latent, key_rope=key_rope, key_up=key_up, value_up=value_up, out_proj=out_proj, norm_gain=norm_gain, routes=routes, route_weight=route_weight, w_gate=w_gate, w_up=w_up, w_down=w_down)


EPSILON = 1e-06
ROPE_BASE = 10000.0

def rotary(values, positions):
    half_width = values.shape[-1] // 2
    inverse = ROPE_BASE ** (-2.0 * jnp.arange(half_width, dtype=jnp.float32) / values.shape[-1])
    angles = positions.astype(jnp.float32)[:, None] * inverse[None, :]
    cosine = jnp.cos(angles)
    sine_part = jnp.sin(angles)
    if values.ndim == 3:
        cosine = cosine[:, None, :]
        sine_part = sine_part[:, None, :]
    first_half = values[..., :half_width]
    second = values[..., half_width:]
    return jnp.concatenate([first_half * cosine - second * sine_part, second * cosine + first_half * sine_part], axis=-1)

def reference(residual, query_nope, query_rope, latent, key_rope, key_up, value_up, out_proj, norm_gain, routes, route_weight, w_gate, w_up, w_down):
    positions = jnp.arange(TOKENS, dtype=jnp.int32)
    query_rot = rotary(query_rope.astype(jnp.float32).reshape(TOKENS, HEADS, QK_ROPE), positions).astype(jnp.bfloat16)
    key_rot = rotary(key_rope.astype(jnp.float32), positions).astype(jnp.bfloat16)
    key_nope = jnp.dot(latent, key_up, preferred_element_type=jnp.float32).astype(jnp.bfloat16)
    value_rows = jnp.dot(latent, value_up, preferred_element_type=jnp.float32).astype(jnp.bfloat16)
    keys_wide = key_nope.astype(jnp.float32).reshape(TOKENS, HEADS, QK_NOPE)
    values_wide = value_rows.astype(jnp.float32).reshape(TOKENS, HEADS, V_DIM)
    rot_wide = key_rot.astype(jnp.float32)
    query_wide = query_nope.astype(jnp.float32).reshape(TOKENS, HEADS, QK_NOPE)
    query_rot_wide = query_rot.astype(jnp.float32)
    score_scale = (QK_NOPE + QK_ROPE) ** (-0.5)
    key_segment = positions // SEGMENT
    query_block = math.gcd(TOKENS, 512)

    def one_block(block_index):
        first_row = (block_index * query_block).astype(jnp.int32)
        query_part = lax.dynamic_slice_in_dim(query_wide, first_row, query_block, 0)
        rot_part = lax.dynamic_slice_in_dim(query_rot_wide, first_row, query_block, 0)
        scores = jnp.einsum('qhd,khd->hqk', query_part, keys_wide)
        scores = (scores + jnp.einsum('qhr,kr->hqk', rot_part, rot_wide)) * score_scale
        query_segment = (first_row + jnp.arange(query_block, dtype=jnp.int32)) // SEGMENT
        allowed = (key_segment[None, :] <= query_segment[:, None])[None]
        scores = jnp.where(allowed, scores, -jnp.inf)
        row_max = lax.optimization_barrier(jnp.max(scores, axis=-1, keepdims=True))
        weights = jnp.exp(scores - row_max)
        weight_sum = lax.optimization_barrier(jnp.sum(weights, axis=-1))
        weights_low = lax.optimization_barrier(weights.astype(jnp.bfloat16)).astype(jnp.float32)
        weighted = jnp.einsum('hqk,khv->qhv', weights_low, values_wide)
        return weighted / weight_sum.T[:, :, None]
    attn_out = lax.map(one_block, jnp.arange(TOKENS // query_block, dtype=jnp.int32))
    attn_out = attn_out.reshape(TOKENS, HEADS * V_DIM).astype(jnp.bfloat16)
    projected = jnp.dot(attn_out, out_proj, preferred_element_type=jnp.float32)
    hidden = (residual.astype(jnp.float32) + projected).astype(jnp.bfloat16)
    hidden_wide = hidden.astype(jnp.float32)
    normed = hidden_wide * lax.rsqrt(lax.optimization_barrier(jnp.mean(hidden_wide * hidden_wide, axis=-1, keepdims=True)) + EPSILON)
    normed = (normed * norm_gain[None, :]).astype(jnp.bfloat16)
    buffer_rows = N_TP * N_SP * CAP
    flat_expert = routes.reshape(-1).astype(jnp.int32)
    onehot = (flat_expert[:, None] == jnp.arange(EXPERTS, dtype=jnp.int32)[None, :]).astype(jnp.int32)
    slot_rank = lax.optimization_barrier(jnp.sum(jnp.cumsum(onehot, axis=0) * onehot, axis=1)) - 1
    slot_index = (flat_expert * buffer_rows + slot_rank).astype(jnp.int32)
    buffer = jnp.zeros((EXPERTS * buffer_rows, D), jnp.bfloat16).at[slot_index].set(jnp.repeat(normed, TOP, axis=0))

    def expert_rows(inputs):
        rows_in, gate_weight, up_weight, down_weight = inputs
        gate_part = jnp.dot(rows_in, gate_weight, preferred_element_type=jnp.float32)
        up_part = jnp.dot(rows_in, up_weight, preferred_element_type=jnp.float32)
        activated = lax.optimization_barrier((jax.nn.silu(gate_part) * up_part).astype(jnp.bfloat16))
        parts = jnp.einsum('bpf,pfd->pbd', activated.astype(jnp.float32).reshape(buffer_rows, N_TP, FF // N_TP), down_weight.astype(jnp.float32).reshape(N_TP, FF // N_TP, D))
        half_out = lax.optimization_barrier(parts.astype(jnp.bfloat16)).astype(jnp.float32)
        return lax.optimization_barrier(jnp.sum(half_out, axis=0)).astype(jnp.bfloat16)
    outputs = lax.map(expert_rows, (buffer.reshape(EXPERTS, buffer_rows, D), w_gate, w_up, w_down))
    picked = outputs.reshape(EXPERTS * buffer_rows, D)[slot_index]
    combined = lax.optimization_barrier(jnp.sum(picked.astype(jnp.float32).reshape(TOKENS, TOP, D) * route_weight[:, :, None], axis=1))
    return (hidden_wide + combined).astype(jnp.bfloat16)
```

```python
import functools

import jax
import jax.numpy as jnp
from jax import lax
from jax.experimental import pallas as pl
from jax.experimental.pallas import tpu as pltpu
from jax.sharding import PartitionSpec as P

QK_NOPE = 128
QK_ROPE = 64
V_DIM = 128
SEGMENT = 64
EPSILON = 1e-06
ROPE_BASE = 10000.0
NEG_LARGE = -1e30
LOG2_E = 1.4426950408889634
MESH = pl.DeviceIdType.MESH
VMEM = pl.BlockSpec(memory_space=pltpu.VMEM)
ANY = pl.BlockSpec(memory_space=pl.ANY)
SIDE = 4
CHIPS = SIDE**3
TILES = 20
ORDERS = ((2, 1, 0), (1, 0, 2), (0, 2, 1))
COLOURS = ((0, 7), (7, 7), (14, 6))


def rotary_parts(positions, width):
    half = width // 2
    inverse = ROPE_BASE ** (-2.0 * jnp.arange(half, dtype=jnp.float32) / width)
    angles = positions.astype(jnp.float32)[:, None] * inverse[None, :]
    return jnp.cos(angles), jnp.sin(angles)


def rotary(values, positions):
    half = values.shape[-1] // 2
    cosine, sine = rotary_parts(positions, values.shape[-1])
    if values.ndim == 3:
        cosine, sine = cosine[:, None, :], sine[:, None, :]
    first, second = values[..., :half], values[..., half:]
    return jnp.concatenate([first * cosine - second * sine, second * cosine + first * sine], axis=-1)


def place():
    sp, tp = lax.axis_index("sp"), lax.axis_index("tp")
    return sp, tp, [sp // (SIDE * SIDE), (sp // SIDE) % SIDE, sp % SIDE]


def chip_of(coords):
    return (coords[0] * SIDE + coords[1]) * SIDE + coords[2]


def moved(coords, axis, by):
    return [lax.rem(c + by + SIDE, SIDE) if a == axis else c for a, c in enumerate(coords)]


def gather_kernel(count, *refs):
    packed, swap_in = refs[0], refs[1 : 1 + count]
    whole, swap_out = refs[1 + count], refs[2 + count : 2 + 2 * count]
    own_sem, send, recv, swap_send, swap_recv = refs[2 + 2 * count :]
    sp, tp, me = place()
    own = pltpu.make_async_copy(packed, whole.at[me[0], me[1], me[2]], own_sem)
    own.start()
    barrier = pltpu.get_barrier_semaphore()
    for axis in range(3):
        for by in (1, -1):
            pl.semaphore_signal(
                barrier, inc=1, device_id=(chip_of(moved(me, axis, by)), tp), device_id_type=MESH
            )
    pl.semaphore_signal(barrier, inc=1, device_id=(sp, 1 - tp), device_id_type=MESH)
    pl.semaphore_wait(barrier, 7)

    def part(coords, done, first, tiles):
        index = [slice(None) if a in done else coords[a] for a in range(3)]
        return whole.at[index[0], index[1], index[2], pl.ds(first, tiles)]

    def copy(piece, sems, axis, by):
        return pltpu.make_async_remote_copy(
            src_ref=piece,
            dst_ref=piece,
            send_sem=send.at[sems],
            recv_sem=recv.at[sems],
            device_id=(chip_of(moved(me, axis, by)), tp),
            device_id_type=MESH,
        )

    def halves(colour):
        first, tiles = COLOURS[colour]
        low = tiles // 2
        return ((first, low), (first + low, tiles - low))

    own.wait()
    swaps = [
        pltpu.make_async_remote_copy(
            src_ref=swap_in[k],
            dst_ref=swap_out[k],
            send_sem=swap_send.at[k],
            recv_sem=swap_recv.at[k],
            device_id=(sp, 1 - tp),
            device_id_type=MESH,
        )
        for k in range(count)
    ]
    for phase in range(3):
        sent = []
        for colour in range(3):
            axis, done = ORDERS[colour][phase], ORDERS[colour][:phase]
            low, high = halves(colour)
            for by, pair in ((1, (low, high)), (-1, (high, low))):
                for kind in range(2):
                    go = copy(part(me, done, *pair[kind]), (colour, phase, kind, (by + 1) // 2), axis, by)
                    go.start()
                    sent.append(go)
        if phase == 0:
            for s in swaps:
                s.start()
        for colour in range(3):
            axis, done = ORDERS[colour][phase], ORDERS[colour][:phase]
            low, high = halves(colour)
            for by, piece in ((1, low), (-1, high)):
                came = part(moved(me, axis, -by), done, *piece)
                copy(came, (colour, phase, 0, (by + 1) // 2), axis, by).wait_recv()
                go = copy(came, (colour, phase, 2, (by + 1) // 2), axis, by)
                go.start()
                sent.append(go)
        for colour in range(3):
            axis, done = ORDERS[colour][phase], ORDERS[colour][:phase]
            low, high = halves(colour)
            for by, near, far in ((1, high, low), (-1, low, high)):
                copy(
                    part(moved(me, axis, -by), done, *near), (colour, phase, 1, (by + 1) // 2), axis, by
                ).wait_recv()
                copy(
                    part(moved(me, axis, -2 * by), done, *far), (colour, phase, 2, (by + 1) // 2), axis, by
                ).wait_recv()
        for go in sent:
            go.wait_send()
    for s in swaps:
        s.wait()


def gather(packed, *swapped):
    count = len(swapped)
    return pl.pallas_call(
        functools.partial(gather_kernel, count),
        out_shape=(
            jax.ShapeDtypeStruct((SIDE, SIDE, SIDE, *packed.shape), packed.dtype),
            *(jax.ShapeDtypeStruct(a.shape, a.dtype) for a in swapped),
        ),
        in_specs=[ANY] * (1 + count),
        out_specs=(VMEM, *([ANY] * count)),
        scratch_shapes=[
            pltpu.SemaphoreType.DMA,
            pltpu.SemaphoreType.DMA((3, 3, 3, 2)),
            pltpu.SemaphoreType.DMA((3, 3, 3, 2)),
            pltpu.SemaphoreType.DMA((count,)),
            pltpu.SemaphoreType.DMA((count,)),
        ],
        compiler_params=pltpu.CompilerParams(collective_id=0, has_side_effects=True),
        name="gather",
    )(packed, *swapped)


def attention_kernel(whole, q_own, q_other, up_own, up_other, out, q_all, keys, values, total, top, mass):
    heads = 8
    queries = q_own.shape[1] // (heads // 2)
    sp, tp = lax.axis_index("sp"), lax.axis_index("tp")
    rows = whole.shape[1] * 128
    top[...] = jnp.full(top.shape, NEG_LARGE, jnp.float32)
    mass[...] = jnp.zeros(mass.shape, jnp.float32)
    total[...] = jnp.zeros(total.shape, jnp.float32)
    last = sp // SIDE

    def group(g, masked):
        for b in range(SIDE):
            block = slice(b * 128, (b + 1) * 128)
            left = whole[g, b, pl.ds(0, 8)].reshape(128, 128)
            right = whole[g, b, pl.ds(8, 8)].reshape(128, 128)
            turned = whole[g, b, pl.ds(16, 4)].reshape(64, 128)
            keys[block, 0:128] = left
            keys[block, 128:256] = right
            keys[b * 128 : b * 128 + 64, 256:384] = turned
            keys[b * 128 + 64 : b * 128 + 128, 256:384] = pltpu.roll(turned, 64, 1)
        values[...] = keys[:, 0:256].T
        if masked:
            row = lax.broadcasted_iota(jnp.int32, (rows, queries), 0)
            column = lax.broadcasted_iota(jnp.int32, (rows, queries), 1)
            key_segment = (g * SIDE + row // 128) * 4 + tp * 2 + (row % 128) // SEGMENT
            allowed = key_segment <= sp * 4 + column // SEGMENT
        for h in range(heads):
            q = (q_own, q_other)[h // 4]
            at = slice((h % 4) * queries, (h % 4 + 1) * queries)
            scores = jnp.dot(keys[...], q[:, at], preferred_element_type=jnp.float32)
            if masked:
                scores = jnp.where(allowed, scores, NEG_LARGE)
            old = top[h : h + 1, :]
            new = jnp.maximum(old, jnp.max(scores, axis=0, keepdims=True))
            weights = jnp.exp2(scores - new)
            shrink = jnp.exp2(old - new)
            top[h : h + 1, :] = new
            mass[h : h + 1, :] = mass[h : h + 1, :] * shrink + jnp.sum(weights, axis=0, keepdims=True)
            product = jnp.dot(values[...], weights.astype(jnp.bfloat16), preferred_element_type=jnp.float32)
            total[h] = total[h] * shrink + product

    group(last, True)
    lax.fori_loop(0, last, lambda g, c: (group(g, False), c)[1], 0)
    for b in range(2):
        first = jnp.where(b == 0, tp, 1 - tp) * 512
        up = (up_own, up_other)[b]
        for h in range(4):
            latent_out = total[b * 4 + h].astype(jnp.bfloat16)
            here = lax.dot_general(
                latent_out, up[:, h * 128 : (h + 1) * 128], (((0,), (0,)), ((), ())), preferred_element_type=jnp.float32
            )
            out[:, pl.ds(pl.multiple_of(first + h * 128, 128), 128)] = here
    stats = jnp.concatenate([top[...], mass[...], jnp.zeros((112, queries), jnp.float32)], axis=0)
    out[:, 1024:1152] = stats.T


def attend(whole, q_own, q_other, up_own, up_other):
    queries = q_own.shape[1] // 4
    return pl.pallas_call(
        attention_kernel,
        out_shape=jax.ShapeDtypeStruct((queries, 1152), jnp.float32),
        in_specs=[VMEM] * 5,
        out_specs=VMEM,
        scratch_shapes=[
            pltpu.VMEM((8, 128), jnp.float32),
            pltpu.VMEM((512, 384), jnp.bfloat16),
            pltpu.VMEM((256, 512), jnp.bfloat16),
            pltpu.VMEM((8, 256, queries), jnp.float32),
            pltpu.VMEM((8, queries), jnp.float32),
            pltpu.VMEM((8, queries), jnp.float32),
        ],
        compiler_params=pltpu.CompilerParams(vmem_limit_bytes=56 * 1024 * 1024),
        name="attend",
    )(whole, q_own, q_other, up_own, up_other)


def exchange_kernel(outgoing, arrived, own_sem, send, recv):
    sp, tp, _ = place()
    barrier = pltpu.get_barrier_semaphore()

    def greet(k, carry):
        pl.semaphore_signal(barrier, inc=1, device_id=(lax.rem(sp + k, CHIPS), tp), device_id_type=MESH)
        return carry

    lax.fori_loop(1, CHIPS, greet, 0)
    own = pltpu.make_async_copy(outgoing.at[sp], arrived.at[sp], own_sem)
    own.start()
    pl.semaphore_wait(barrier, CHIPS - 1)

    def to(k):
        dz, dy, dx = k // 16, (k // 4) % 4, k % 4
        z, y, x = sp // 16, (sp // 4) % 4, sp % 4
        return (lax.rem(z + dz, 4) * 4 + lax.rem(y + dy, 4)) * 4 + lax.rem(x + dx, 4)

    def start(k, carry):
        peer = to(k)
        pltpu.make_async_remote_copy(
            src_ref=outgoing.at[peer],
            dst_ref=arrived.at[sp],
            send_sem=send,
            recv_sem=recv,
            device_id=(peer, tp),
            device_id_type=MESH,
        ).start()
        return carry

    lax.fori_loop(1, CHIPS, start, 0)
    own.wait()
    most = pl.ds(0, CHIPS - 1)
    every = pltpu.make_async_remote_copy(
        src_ref=outgoing.at[most],
        dst_ref=arrived.at[most],
        send_sem=send,
        recv_sem=recv,
        device_id=(sp, 1 - tp),
        device_id_type=MESH,
    )
    every.wait_send()
    every.wait_recv()


def exchange(outgoing, number):
    return pl.pallas_call(
        exchange_kernel,
        out_shape=jax.ShapeDtypeStruct(outgoing.shape, outgoing.dtype),
        in_specs=[ANY],
        out_specs=ANY,
        scratch_shapes=[pltpu.SemaphoreType.DMA, pltpu.SemaphoreType.DMA, pltpu.SemaphoreType.DMA],
        compiler_params=pltpu.CompilerParams(collective_id=number, has_side_effects=True),
        name=f"exchange{number}",
    )(outgoing)


def local(
    residual,
    query_nope,
    query_rope,
    latent,
    key_rope,
    key_up,
    value_up,
    out_proj,
    norm_gain,
    routes,
    route_weight,
    w_gate,
    w_up,
    w_down,
):
    tp = lax.axis_index("tp")
    sp = lax.axis_index("sp")
    row_count = residual.shape[0]
    queries = query_nope.shape[0]
    heads_here = query_nope.shape[1] // QK_NOPE
    scale = (QK_NOPE + QK_ROPE) ** (-0.5) * LOG2_E
    query_first = sp * queries
    query_pos = query_first + jnp.arange(queries, dtype=jnp.int32)
    query_rot = rotary(query_rope.astype(jnp.float32).reshape(queries, heads_here, QK_ROPE), query_pos)
    rot_side = jnp.transpose(query_rot * scale, (2, 1, 0)).astype(jnp.bfloat16).reshape(QK_ROPE, -1)
    latent_side = jnp.einsum(
        "lhd,qhd->lhq",
        key_up.reshape(-1, heads_here, QK_NOPE),
        query_nope.reshape(queries, heads_here, QK_NOPE),
        preferred_element_type=jnp.float32,
    )
    latent_side = (latent_side * scale).astype(jnp.bfloat16).reshape(latent_side.shape[0], -1)
    q_own = jnp.concatenate([latent_side, rot_side, jnp.zeros_like(rot_side)], axis=0)
    key_pos = query_first + tp * row_count + jnp.arange(row_count, dtype=jnp.int32)
    key_rot = rotary(key_rope.astype(jnp.float32), key_pos).astype(jnp.bfloat16)
    packed = jnp.concatenate(
        [
            latent[:, :128].reshape(8, 16, 128),
            latent[:, 128:].reshape(8, 16, 128),
            jnp.concatenate([key_rot[:64], key_rot[64:]], axis=1).reshape(4, 16, 128),
        ],
        axis=0,
    )
    gate_own, up_own, down_own = w_gate[0], w_up[0], w_down[0]
    whole, q_other, value_other, gate_other, up_other, down_other = gather(
        packed, q_own, value_up, gate_own, up_own, down_own
    )
    partial = attend(whole.reshape(SIDE * SIDE, SIDE, TILES, 16, 128), q_own, q_other, value_up, value_other)
    both = lax.all_to_all(
        partial.reshape(2, row_count, 1152), "tp", split_axis=0, concat_axis=0, tiled=True
    )
    order = jnp.arange(2, dtype=jnp.int32)[:, None, None]

    def by_head(stats):
        return jnp.where(order == 0, stats, jnp.concatenate([stats[..., 4:], stats[..., :4]], axis=-1))

    top, mass = by_head(both[:, :, 1024:1032]), by_head(both[:, :, 1032:1040])
    factor = jnp.exp2(top - jnp.max(top, axis=0, keepdims=True))
    factor = factor / jnp.sum(factor * mass, axis=0, keepdims=True)
    weighted = both[:, :, :1024].reshape(2, row_count, 8, V_DIM)
    attn_out = jnp.sum(weighted * factor[..., None], axis=0).astype(jnp.bfloat16).reshape(row_count, 1024)
    projected = jnp.dot(attn_out, out_proj, preferred_element_type=jnp.float32)
    hidden_wide = residual.astype(jnp.float32) + projected
    hidden = hidden_wide.astype(jnp.bfloat16)
    hidden_wide = hidden.astype(jnp.float32)
    normed = hidden_wide * lax.rsqrt(
        jnp.mean(hidden_wide * hidden_wide, axis=-1, keepdims=True) + EPSILON
    )
    normed = (normed * norm_gain[None, :]).astype(jnp.bfloat16)
    expert_count = CHIPS
    capacity = 8
    top_count = routes.shape[1]
    width = normed.shape[1]
    flat_expert = routes.reshape(-1)
    onehot = (flat_expert[:, None] == jnp.arange(expert_count, dtype=jnp.int32)[None, :]).astype(
        jnp.int32
    )
    slot_rank = jnp.sum(jnp.cumsum(onehot, axis=0) * onehot, axis=1) - 1
    slot_index = flat_expert * capacity + slot_rank
    outgoing = (
        jnp.zeros((expert_count * capacity, width), jnp.bfloat16)
        .at[slot_index]
        .set(jnp.repeat(normed, top_count, axis=0))
    )
    rows = exchange(outgoing.reshape(expert_count, capacity, width), 1).reshape(-1, width)

    def half(gate, up, down):
        gate_part = jnp.dot(rows, gate, preferred_element_type=jnp.float32)
        up_part = jnp.dot(rows, up, preferred_element_type=jnp.float32)
        activated = (jax.nn.silu(gate_part) * up_part).astype(jnp.bfloat16)
        return jnp.dot(activated, down, preferred_element_type=jnp.float32)

    expert_out = (half(gate_own, up_own, down_own) + half(gate_other, up_other, down_other)).astype(jnp.bfloat16)
    back_rows = exchange(expert_out.reshape(expert_count, capacity, width), 2)
    picked = back_rows.reshape(expert_count * capacity, width)[slot_index]
    combined = jnp.sum(
        picked.astype(jnp.float32).reshape(row_count, top_count, width) * route_weight[:, :, None],
        axis=1,
    )
    return (hidden_wide + combined).astype(jnp.bfloat16)


def solution(mesh):
    return jax.shard_map(
        local,
        mesh=mesh,
        in_specs=(
            P(("sp", "tp"), None),
            P("sp", "tp"),
            P("sp", "tp"),
            P(("sp", "tp"), None),
            P(("sp", "tp"), None),
            P(None, "tp"),
            P(None, "tp"),
            P(),
            P(),
            P(("sp", "tp"), None),
            P(("sp", "tp"), None),
            P("sp", None, "tp"),
            P("sp", None, "tp"),
            P("sp", "tp", None),
        ),
        out_specs=P(("sp", "tp"), None),
        check_vma=False,
    )
```
